512 devices in a mesh: rep: 2 (over z_hi), fs: 32 (over z_lo, y), tp: 8 (over x, core).
Axes of the slice: x: 4, y: 4, z: 16 (z_hi: 2, z_lo: 8; z = z_hi * 8 + z_lo), core: 2. Of those that a mesh axis runs over, the one named last changes fastest.
Arguments:
- gate_late: bfloat16 [24576, 4096], P(('rep', 'fs'), 'tp'), may hold values from -6 to 6
- up_late: bfloat16 [24576, 4096], P(('rep', 'fs'), 'tp'), may hold values from -6 to 6
- gate_early: bfloat16 [24576, 4096], P(('rep', 'fs'), 'tp'), may hold values from -6 to 6
- up_early: bfloat16 [24576, 4096], P(('rep', 'fs'), 'tp'), may hold values from -6 to 6
- cotangent: bfloat16 [24576, 2048], P(('rep', 'fs')), may hold values from -16 to 16
- w_down: bfloat16 [2048, 4096], P('fs', 'tp'), may hold values from -0.09375 to 0.09375
- grad_in: float32 [2048, 4096], P('fs', 'tp'), may hold values from -6 to 6
Outputs:
- late_out: bfloat16 [24576, 2048], P(('rep', 'fs'))
- gate_grad: bfloat16 [24576, 4096], P(('rep', 'fs'), 'tp')
- up_grad: bfloat16 [24576, 4096], P(('rep', 'fs'), 'tp')
- grad_out: float32 [2048, 4096], P('fs', 'tp')
The draws below stay inside these ranges and needn't reach their ends.
All inputs are finite; a program needn't handle non-finite values.
Results may differ from the reference program's by a relative error of at most 0.014.
Values may be sent and summed in bfloat16 or wider, within the bound.
No kernel may reach another device: no remote copies, remote signals or barrier semaphores. Data moves between devices by JAX's collectives and lax.ppermute only.
A program may use at most 64 MiB of HBM per device.

```python
import jax
import jax.numpy as jnp
from jax import lax

D = 2048
FF = 4096
TOKENS = 24576
N_TP = 8


def spiked(result, own_key, source, target, blocks, factor):
    def block_of(position):
        return (jnp.arange(result.shape[position]) // (result.shape[position] // blocks)).reshape((-1,) + (1,) * (result.ndim - 1 - position))

    one_side = jax.random.permutation(own_key, blocks)[block_of(target)]
    other_side = (block_of(target) + blocks // 2) % blocks
    return jnp.where((block_of(source) == one_side) | (block_of(source) == other_side), factor * result, result)


def steps_of(own_key, extent, shards, smallest, largest):
    gain = 1.0
    for position, blocks in shards:
        steps = jax.random.uniform(jax.random.fold_in(jax.random.fold_in(own_key, 6), position), (blocks,), jnp.float32, smallest / len(shards), largest / len(shards))
        gain = gain * jnp.repeat(jnp.exp(steps), extent[position] // blocks).reshape((-1,) + (1,) * (len(extent) - 1 - position))
    return gain


def normal_values(key, dims, deviation, limit, pieces=(), kind=jnp.bfloat16):
    loudness = steps_of(key, dims, pieces, -0.22, 0.18) if pieces else 1.0
    result = jax.random.normal(key, dims, jnp.float32) * deviation * loudness
    return jnp.minimum(jnp.maximum(result, -limit), limit).astype(kind)


def gaussian_with(stream_key, shape, width, reach, cuts, heavy, kind=jnp.bfloat16):
    drawn = width * jax.random.normal(stream_key, shape, jnp.float32)
    if cuts:
        drawn = drawn * steps_of(stream_key, shape, cuts, -0.22, 0.18)
    return jnp.clip(spiked(drawn, jax.random.fold_in(stream_key, 3), *heavy), -reach, reach).astype(kind)


def setup_inputs(seed: int = 0) -> dict:
    splits = jax.random.split(jax.random.key(seed), 8)
    return {
        "gate_late": normal_values(splits[0], (TOKENS, FF), 1.0, 6.0, ((0, 64), (1, 8))),
        "up_late": normal_values(splits[1], (TOKENS, FF), 1.0, 6.0, ((0, 64), (1, 8))),
        "gate_early": normal_values(splits[2], (TOKENS, FF), 1.0, 6.0, ((0, 64), (1, 8))),
        "up_early": normal_values(splits[3], (TOKENS, FF), 1.0, 6.0, ((0, 64), (1, 8))),
        "cotangent": gaussian_with(splits[4], (TOKENS, D), 1.0, 16.0, ((0, 64),), (0, 1, 64, 4.0)),
        "w_down": normal_values(splits[5], (D, FF), FF ** -0.5, 0.09375, ((0, 32), (1, 8))),
        "grad_in": normal_values(splits[6], (D, FF), 1.0, 6.0, ((0, 32), (1, 8)), jnp.float32),
    }


def reference(gate_late, up_late, gate_early, up_early, cotangent, w_down, grad_in):
    gate_value = gate_late.astype(jnp.float32)
    hidden_late = (jax.nn.silu(gate_value) * up_late.astype(jnp.float32)).astype(jnp.bfloat16)
    block_width = FF // N_TP

    def add_block(block_index, running):
        offset = (block_index * block_width).astype(jnp.int32)
        hidden_block = lax.dynamic_slice_in_dim(hidden_late, offset, block_width, 1)
        weight_block = lax.dynamic_slice_in_dim(w_down, offset, block_width, 1)
        partial_value = lax.dot_general(hidden_block, weight_block, (((1,), (1,)), ((), ())), preferred_element_type=jnp.float32)
        rounded = lax.optimization_barrier(partial_value.astype(jnp.bfloat16))
        return running + rounded.astype(jnp.float32)
    summed = lax.fori_loop(0, N_TP, add_block, jnp.zeros((gate_late.shape[0], D), jnp.float32))
    late_out = summed.astype(jnp.bfloat16)
    gate_value = gate_early.astype(jnp.float32)
    sigmoid_early = jax.nn.sigmoid(gate_value)
    swish_early = gate_value * sigmoid_early
    up_value = up_early.astype(jnp.float32)
    hidden_early = (swish_early * up_value).astype(jnp.bfloat16)
    hidden_grad = jnp.dot(cotangent, w_down, preferred_element_type=jnp.float32)
    gate_grad = (hidden_grad * up_value * sigmoid_early * (1.0 + gate_value * (1.0 - sigmoid_early))).astype(jnp.bfloat16)
    up_grad = (hidden_grad * swish_early).astype(jnp.bfloat16)
    weight_grad = lax.dot_general(cotangent, hidden_early, (((0,), (0,)), ((), ())), preferred_element_type=jnp.float32)
    grad_out = grad_in + weight_grad * (1.0 / jnp.sqrt(jnp.float32(TOKENS)))
    return (late_out, gate_grad, up_grad, grad_out)
```

```python
import functools
import math

import jax
import jax.numpy as jnp
from jax import lax
from jax.experimental import pallas as pl
from jax.experimental.pallas import tpu as pltpu
from jax.sharding import Mesh
from jax.sharding import PartitionSpec as P


Z = ("zh", "zl")
FS = ("zl", "y")
REP_FS = ("zh", "zl", "y")
TP = ("x", "c")
NY = 4
NZ = 8
NX = 4
F32 = jnp.float32
BF16 = jnp.bfloat16
VM = pl.BlockSpec(memory_space=pltpu.VMEM)
SM = pl.BlockSpec(memory_space=pltpu.SMEM)


def call(body, outs, ins, scratch=(), flops=0, moved=0, name=None):
    return pl.pallas_call(
        body,
        out_shape=outs,
        in_specs=ins,
        out_specs=tuple(VM for _ in outs),
        scratch_shapes=scratch,
        cost_estimate=pl.CostEstimate(flops=flops, bytes_accessed=moved, transcendentals=0),
        compiler_params=pltpu.CompilerParams(vmem_limit_bytes=32 * 1024 * 1024),
        name=name,
    )


def shape(dims, dtype):
    return jax.ShapeDtypeStruct(dims, dtype)


def sigmoid(v):
    return 1.0 / (1.0 + jnp.exp(-v))


def gated(gate, up):
    gate = gate.astype(F32)
    return (gate * sigmoid(gate) * up.astype(F32)).astype(BF16)


def weight_grad_body(cot, gate, up, out):
    hidden = gated(gate[...], up[...])
    rows = out.shape[2]
    for k in range(NZ):
        part = lax.dot_general(
            cot[:, k * NY * rows : (k + 1) * NY * rows],
            hidden,
            (((0,), (0,)), ((), ())),
            preferred_element_type=F32,
        )
        out[:, k] = part.astype(BF16).reshape(NY, rows, -1)


def y_sum_body(z, parts, minus, own, plus):
    for j in range(NZ):
        k = lax.rem(z[0] + j + NZ // 2, NZ)
        total = parts[0, k].astype(F32)
        for y in range(1, NY):
            total += parts[y, k].astype(F32)
        if j < 3:
            minus[j] = total.astype(BF16)
        elif j < 6:
            own[j - 3] = total
        else:
            plus[j - 6] = total.astype(BF16)


def triple_body(own, from_minus, from_plus, down, mid, up):
    down[...] = (own[0] + from_minus[0].astype(F32) + from_plus[0].astype(F32)).astype(BF16)
    mid[...] = own[1] + from_minus[1].astype(F32) + from_plus[1].astype(F32)
    up[...] = (own[2] + from_plus[2].astype(F32)).astype(BF16)


def near_body(mid, one, two, out):
    out[...] = (mid[...] + one[...].astype(F32) + two[...].astype(F32)).astype(BF16)


def final_body(scale, grad, near, far, out):
    out[...] = grad[...] + (near[...].astype(F32) + far[...].astype(F32)) * scale


def join_body(below, own, above, three, two):
    three[0] = below[...]
    three[1] = own[...]
    three[2] = above[...]
    two[0] = below[...]
    two[1] = own[...]


def spread_body(z, low, mid, high, out):
    for j in range(NZ):
        k = lax.rem(z[0] + j + NZ // 2, NZ)
        block = low[j] if j < 3 else mid[j - 3] if j < 6 else high[j - 6]
        for y in range(NY):
            out[y, k] = block


def late_body(core, gate, up, weights, mine, other, hidden):
    hidden[...] = gated(gate[...], up[...])
    half, wide = mine.shape
    step = wide // NZ
    first = pl.multiple_of(core[0] * half, half)
    second = pl.multiple_of((1 - core[0]) * half, half)
    for out, start in ((other, second), (mine, first)):
        rows = hidden[pl.ds(start, half), :]
        for k in range(NZ):
            block = weights[:, k].reshape(step, -1)
            part = lax.dot_general(rows, block, (((1,), (1,)), ((), ())), preferred_element_type=F32)
            out[:, k * step : (k + 1) * step] = part.astype(BF16)


def pair_body(one, two, out):
    out[...] = (one[...].astype(F32) + two[...].astype(F32)).astype(BF16)


def x_sum_body(parts, out):
    total = parts[0].astype(F32)
    for x in range(1, NX):
        total += parts[x].astype(F32)
    total = total.astype(BF16)
    for x in range(NX):
        out[x] = total


def place_body(core, mine, other, out):
    half = mine.shape[0]
    out[pl.ds(pl.multiple_of(core[0] * half, half), half), :] = mine[...]
    out[pl.ds(pl.multiple_of((1 - core[0]) * half, half), half), :] = other[...]


def early_body(cot, gate, up, weights, gate_grad, up_grad, total):
    step = cot.shape[1] // NZ
    for k in range(NZ):
        part = jnp.dot(
            cot[:, k * step : (k + 1) * step], weights[:, k].reshape(step, -1), preferred_element_type=F32
        )
        if k == 0:
            total[...] = part
        else:
            total[...] += part
    g = gate[...].astype(F32)
    s = sigmoid(g)
    h = total[...]
    gate_grad[...] = (h * up[...].astype(F32) * s * (1.0 + g * (1.0 - s))).astype(BF16)
    up_grad[...] = (h * (g * s)).astype(BF16)


def shifted(x, axis, by):
    n = lax.axis_size(axis)
    return lax.ppermute(x, axis, [(i, (i + by) % n) for i in range(n)])


def exchanged(x, axis):
    return lax.all_to_all(x, axis, 0, 0, tiled=True)


def per_device(gate_late, up_late, gate_early, up_early, cotangent, w_down, grad_in):
    tokens, ff = gate_late.shape
    rows = w_down.shape[0]
    wide = cotangent.shape[1]
    flops = 2 * tokens * wide * ff
    z = lax.axis_index("zl").astype(jnp.int32).reshape(1)
    core = lax.axis_index("c").astype(jnp.int32).reshape(1)
    scale = 1.0 / math.sqrt(tokens * lax.axis_size(REP_FS))

    above = shifted(w_down, Z, -1)
    below = shifted(w_down, Z, 1)
    (grads,) = call(
        weight_grad_body, (shape((NY, NZ, rows, ff), BF16),), [VM] * 3, flops=flops, moved=5 << 20
    )(cotangent, gate_early, up_early)
    three, two = call(
        join_body, (shape((3, rows, ff), BF16), shape((2, rows, ff), BF16)), [VM] * 3, moved=1 << 19
    )(below, w_down, above)
    low = shifted(three, Z, 3)
    high = shifted(two, Z, -3)
    grads = exchanged(grads, "y")
    (spread,) = call(spread_body, (shape((NY, NZ, rows, ff), BF16),), [SM, VM, VM, VM], moved=5 << 19)(
        z, low, three, high
    )
    weights = exchanged(spread, "y")

    minus, own, plus = call(
        y_sum_body,
        (shape((3, rows, ff), BF16), shape((3, rows, ff), F32), shape((2, rows, ff), BF16)),
        [SM, VM],
        moved=3 << 20,
    )(z, grads)
    from_plus = shifted(minus, Z, -3)
    from_minus = shifted(plus, Z, 3)
    down, mid, up = call(
        triple_body,
        (shape((rows, ff), BF16), shape((rows, ff), F32), shape((rows, ff), BF16)),
        [VM] * 3,
        moved=1 << 20,
    )(own, from_minus, from_plus)
    one = shifted(up, Z, 1)
    other_one = shifted(down, Z, -1)
    (near,) = call(near_body, (shape((rows, ff), BF16),), [VM] * 3, moved=3 << 17)(mid, one, other_one)
    far = shifted(near, Z, NZ)
    (grad_out,) = call(
        functools.partial(final_body, scale), (shape((rows, ff), F32),), [VM] * 3, moved=3 << 17
    )(grad_in, near, far)

    half = tokens // 2
    mine, theirs = call(
        late_body,
        (shape((half, wide), BF16), shape((half, wide), BF16)),
        [SM, VM, VM, VM],
        scratch=[pltpu.VMEM((tokens, ff), BF16)],
        flops=flops,
        moved=5 << 20,
    )(core, gate_late, up_late, weights)
    theirs = shifted(theirs, "c", 1)
    (paired,) = call(pair_body, (shape((half, wide), BF16),), [VM] * 2, moved=9 << 18)(mine, theirs)
    parts = exchanged(paired.reshape(NX, half // NX, wide), "x")
    (sums,) = call(x_sum_body, (shape((NX, half // NX, wide), BF16),), [VM], moved=3 << 19)(parts)
    own_half = exchanged(sums, "x").reshape(half, wide)
    other_half = shifted(own_half, "c", 1)
    (late_out,) = call(place_body, (shape((tokens, wide), BF16),), [SM, VM, VM], moved=3 << 20)(
        core, own_half, other_half
    )

    gate_grad, up_grad = call(
        early_body,
        (shape((tokens, ff), BF16), shape((tokens, ff), BF16)),
        [VM] * 4,
        scratch=[pltpu.VMEM((tokens, ff), F32)],
        flops=flops,
        moved=6 << 20,
    )(cotangent, gate_early, up_early, weights)
    return (late_out, gate_grad, up_grad, grad_out)


def solution(mesh):
    torus = Mesh(mesh.devices.reshape(2, NZ, NY, NX, 2), ("zh", "zl", "y", "x", "c"))
    return jax.shard_map(
        per_device,
        mesh=torus,
        in_specs=(
            P(REP_FS, TP),
            P(REP_FS, TP),
            P(REP_FS, TP),
            P(REP_FS, TP),
            P(REP_FS, None),
            P(FS, TP),
            P(FS, TP),
        ),
        out_specs=(P(REP_FS, None), P(REP_FS, TP), P(REP_FS, TP), P(FS, TP)),
        check_vma=False,
    )
```
